32 devices in a mesh: grp: 2 (over y), sp: 4 (over z), tp: 4 (over x, core).
Axes of the slice: x: 2, y: 2, z: 4, core: 2. Of those that a mesh axis runs over, the one named last changes fastest.
Arguments:
- queries: bfloat16 [2048, 2048], P(('grp', 'sp'), 'tp'), parts along dimension 0, may hold values from -6 to 6
- keys: bfloat16 [2048, 2048], P(('grp', 'sp'), 'tp'), parts along dimension 0, may hold values from -6 to 6
- values: bfloat16 [2048, 2048], P(('grp', 'sp'), 'tp'), parts along dimension 0, may hold values from -8 to 8
- offsets: float32 [16], P('tp'), as said below
- residual: bfloat16 [2048, 4096], P(('grp', 'sp', 'tp')), parts along dimension 0, may hold values from -6 to 6
- out_weight: bfloat16 [2048, 4096], P('tp'), may hold values from -0.52734375 to 0.52734375
- gain_one: float32 [4096], replicated, may hold values from 0.1 to 1.9
- shift_one: float32 [4096], replicated, may hold values from -3 to 3
- gain_two: float32 [4096], replicated, may hold values from 0.1 to 1.9
- shift_two: float32 [4096], replicated, may hold values from -3 to 3
- group_prob: float32 [2048], P(('grp', 'sp', 'tp')), parts along dimension 0, may hold values from 0.2 to 1
- pair_logits: float32 [2048, 2], P(('grp', 'sp', 'tp')), parts along dimension 0, may hold values from -6 to 6
- routes: int32 [2048, 2], P(('grp', 'sp', 'tp')), parts along dimension 0, may hold values from 0 to 15, as said below
- w_gate: bfloat16 [16, 4096, 256], P(('sp', 'tp')), may hold values from -0.09375 to 0.09375
- w_up: bfloat16 [16, 4096, 256], P(('sp', 'tp')), may hold values from -0.09375 to 0.09375
- w_down: bfloat16 [16, 256, 4096], P(('sp', 'tp')), may hold values from -1.5 to 1.5
Outputs:
- layer_out: bfloat16 [2048, 4096], P(('grp', 'sp', 'tp')), parts along dimension 0
The draws below stay inside these ranges and needn't reach their ends.
There are 2 independent parts, one for each index of `grp`. The reference program is written for one: setup_inputs(seed, part) draws one part's arguments, and reference() takes and returns one part's arrays. A program takes and returns all parts, laid end to end along the dimension named above; an argument that names none is the same for every part. Nothing has to cross between parts.
Inputs may be any that keep to these rules, and one draw needn't show every extreme that they name: `routes`: both experts of a token are different and lie in one group of 4 consecutive experts. Of the tokens of one device (64 consecutive ones), at most 16 name any one expert; in every draw some experts are named exactly 16 times by the tokens of every device. `offsets`: each offset lies between 2.5 and ln(1024) - 0.3.
All inputs are finite; a program needn't handle non-finite values.
Results may differ from the reference program's by a relative error of at most 0.014.
Values may be sent and summed in bfloat16 or wider, within the bound.
A program may use at most 128 MiB of HBM per device.

```python
import math
import jax
import jax.numpy as jnp
from jax import lax

D = 4096
HEADS = 16
HEAD_DIM = 128
FE = 256
GROUPS = 4
TOPK = 2
TOK_DEV = 256
TOKENS = 1024
ROWS = 64
EXPERTS = 16
EPG = 4
CAP = 16
N_SP = 4
N_TP = 4


def draw_offsets(key, part):
    upper = math.log(TOKENS) - 0.3
    slow_key, near_key, wide_key = jax.random.split(key, 3)
    slow = jax.random.uniform(slow_key, (HEADS,), jnp.float32) < 0.5
    near = jax.random.uniform(near_key, (HEADS,), jnp.float32, upper - 1.0, upper)
    wide = jnp.exp(jax.random.uniform(wide_key, (HEADS,), jnp.float32, math.log(2.5), math.log(upper - 1.0)))
    return jnp.where(slow, near, wide)


def draw_values(key, part):
    blocks = TOKENS // TOK_DEV
    width = HEADS * HEAD_DIM
    noise_key, mean_key = jax.random.split(jax.random.fold_in(key, 21))
    noise = jax.random.normal(noise_key, (blocks, TOK_DEV, width), jnp.float32)
    means = 2.0 * jax.random.normal(mean_key, (blocks, 1, width), jnp.float32)
    whole = jnp.clip(noise + means, -8.0, 8.0)
    return whole.reshape(TOKENS, width).astype(jnp.bfloat16)


def draw_routes(key, part):
    blocks = TOKENS // ROWS
    busy = jax.random.randint(jax.random.fold_in(key, 11), (), 0, GROUPS)

    def one_block(block_key):
        first_key, second_key, third_key, fourth_key = jax.random.split(block_key, 4)
        order = jax.random.permutation(first_key, ROWS)
        others = (busy + 1 + jax.random.randint(second_key, (ROWS,), 0, GROUPS - 1)) % GROUPS
        group = jnp.where(order < ROWS // 2, busy, others)
        onehot = (group[:, None] == jnp.arange(GROUPS)[None, :]).astype(jnp.int32)
        rank = jnp.sum((jnp.cumsum(onehot, axis=0) - onehot) * onehot, axis=1)
        start = jax.random.randint(third_key, (GROUPS,), 0, EPG)
        stride = jax.random.randint(fourth_key, (GROUPS,), 1, EPG)
        first = (start[group] + rank) % EPG
        second = (start[group] + rank + stride[group]) % EPG
        return jnp.stack([group * EPG + first, group * EPG + second], axis=1)
    block_keys = jax.random.split(jax.random.fold_in(key, 12), blocks)
    return jax.vmap(one_block)(block_keys).reshape(TOKENS, TOPK).astype(jnp.int32)


def shard_levels(own_key, extent, cuts, low, top_value):
    level = 1.0
    for dim, blocks in cuts:
        heights = jax.random.uniform(jax.random.fold_in(jax.random.fold_in(own_key, 6), dim), (blocks,), jnp.float32, low / len(cuts), top_value / len(cuts))
        level = level * jnp.repeat(jnp.exp(heights), extent[dim] // blocks).reshape((-1,) + (1,) * (len(extent) - 1 - dim))
    return level


def bell_draw(stream_key, shape, spread, reach, cuts=(), kind=jnp.bfloat16):
    loudness = shard_levels(stream_key, shape, cuts, -0.22, 0.18) if cuts else 1.0
    values = jax.random.normal(stream_key, shape, jnp.float32) * spread * loudness
    return jnp.minimum(jnp.maximum(values, -reach), reach).astype(kind)


def setup_inputs(seed: int = 0, part: int = 0) -> dict:
    key_list = jax.random.split(jax.random.key(seed), 17)
    own_keys = jax.random.split(jax.random.fold_in(key_list[16], part), 17)
    queries = bell_draw(own_keys[0], (TOKENS, HEADS * HEAD_DIM), 1.0, 6.0, ((0, 4), (1, 4)))
    keys = bell_draw(own_keys[1], (TOKENS, HEADS * HEAD_DIM), 1.0, 6.0, ((0, 4), (1, 4)))
    values = draw_values(jax.random.fold_in(jax.random.fold_in(key_list[16], part), 71), part)
    offsets = draw_offsets(jax.random.fold_in(key_list[16], 71), part)
    residual = bell_draw(own_keys[4], (TOKENS, D), 1.0, 6.0, ((0, 16),))
    out_weight = bell_draw(key_list[5], (HEADS * HEAD_DIM, D), (4.0 / (HEADS * HEAD_DIM) ** 0.5), 0.52734375, ((0, 4),))
    gain_one = jnp.clip(1.0 + 0.18 * jax.random.normal(key_list[6], (D,), jnp.float32), 0.1, 1.9)
    shift_one = bell_draw(key_list[7], (D,), 0.5, 3.0, (), jnp.float32)
    gain_two = jnp.clip(1.0 + 0.18 * jax.random.normal(key_list[8], (D,), jnp.float32), 0.1, 1.9)
    shift_two = bell_draw(key_list[9], (D,), 0.5, 3.0, (), jnp.float32)
    group_prob = jnp.clip(0.2 + 0.8 * jax.random.uniform(own_keys[10], (TOKENS,), jnp.float32) ** shard_levels(own_keys[10], (TOKENS,), ((0, 16),), -0.2, 0.2), 0.2, 1.0)
    pair_logits = bell_draw(own_keys[11], (TOKENS, TOPK), 1.5, 6.0, ((0, 16),), jnp.float32)
    routes = draw_routes(jax.random.fold_in(jax.random.fold_in(key_list[16], part), 71), part)
    w_gate = bell_draw(key_list[13], (EXPERTS, D, FE), D ** -0.5, 0.09375, ((0, 16),))
    w_up = bell_draw(key_list[14], (EXPERTS, D, FE), D ** -0.5, 0.09375, ((0, 16),))
    w_down = bell_draw(key_list[15], (EXPERTS, FE, D), (4.0 / FE ** 0.5), 1.5, ((0, 16),))
    return dict(queries=queries, keys=keys, values=values, offsets=offsets, residual=residual, out_weight=out_weight, gain_one=gain_one, shift_one=shift_one, gain_two=gain_two, shift_two=shift_two, group_prob=group_prob, pair_logits=pair_logits, routes=routes, w_gate=w_gate, w_up=w_up, w_down=w_down)


residual_scale = 8.0 ** 0.25
norm_eps = 1e-05

def layer_norm(rows, gain, shift):
    mean = lax.optimization_barrier(jnp.mean(rows, axis=-1, keepdims=True))
    centred = rows - mean
    variance = lax.optimization_barrier(jnp.mean(centred * centred, axis=-1, keepdims=True))
    return centred * lax.rsqrt(variance + norm_eps) * gain + shift

def slot_index(routes, expert_count, capacity):
    flat = routes.reshape(-1)
    onehot = (flat[:, None] == jnp.arange(expert_count, dtype=jnp.int32)[None, :]).astype(jnp.int32)
    earlier = jnp.cumsum(onehot, axis=0) - onehot
    rank = lax.optimization_barrier(jnp.sum(earlier * onehot, axis=1))
    return (flat * capacity + rank).astype(jnp.int32)

def attend(queries, keys, values, offsets):
    head_count = offsets.shape[0]
    query_heads = queries.reshape(TOKENS, head_count, HEAD_DIM)
    key_heads = keys.reshape(TOKENS, head_count, HEAD_DIM).astype(jnp.float32)
    value_heads = values.reshape(TOKENS, head_count, HEAD_DIM).astype(jnp.float32)
    key_pos = jnp.arange(TOKENS, dtype=jnp.int32)

    def block(index):
        start = (index * TOK_DEV).astype(jnp.int32)
        query_block = lax.dynamic_slice_in_dim(query_heads, start, TOK_DEV, 0).astype(jnp.float32)
        score = jnp.einsum('qhd,khd->hqk', query_block, key_heads) * HEAD_DIM ** (-0.5) - offsets[:, None, None]
        query_pos = start + jnp.arange(TOK_DEV, dtype=jnp.int32)
        strict = key_pos[None, :] < query_pos[:, None]
        keep = jnp.where(strict, jax.nn.log_sigmoid(-score), 0.0)
        later = lax.cumsum(keep, axis=2, reverse=True) - keep
        weight = jnp.where(strict, jnp.exp(jax.nn.log_sigmoid(score) + later), 0.0).astype(jnp.bfloat16)
        weight = lax.optimization_barrier(weight).astype(jnp.float32)
        return jnp.einsum('hqk,khd->qhd', weight, value_heads).astype(jnp.bfloat16)
    out = lax.map(block, jnp.arange(N_SP, dtype=jnp.int32))
    return out.reshape(TOKENS, head_count * HEAD_DIM)

def expert_rows(operands):
    rows, gate_w, up_w, down_w = operands
    gate = jnp.dot(rows, gate_w, preferred_element_type=jnp.float32)
    upper = jnp.dot(rows, up_w, preferred_element_type=jnp.float32)
    hidden = (jax.nn.silu(gate) * upper).astype(jnp.bfloat16)
    return jnp.dot(hidden, down_w, preferred_element_type=jnp.float32).astype(jnp.bfloat16)

def reference(queries, keys, values, offsets, residual, out_weight, gain_one, shift_one, gain_two, shift_two, group_prob, pair_logits, routes, w_gate, w_up, w_down):
    attended = attend(queries, keys, values, offsets)
    span = HEADS * HEAD_DIM // N_TP
    mixed = jnp.zeros((TOKENS, D), jnp.float32)
    for member in range(N_TP):
        partial_sum = jnp.dot(attended[:, member * span:(member + 1) * span], out_weight[member * span:(member + 1) * span], preferred_element_type=jnp.float32)
        partial_sum = lax.optimization_barrier(partial_sum.astype(jnp.bfloat16))
        mixed = mixed + partial_sum.astype(jnp.float32)
    normed = layer_norm(residual_scale * residual.astype(jnp.float32) + mixed, gain_one, shift_one).astype(jnp.bfloat16)
    sources = TOKENS // ROWS
    src_rows = normed.reshape(sources, ROWS, D)
    slots = jax.vmap(lambda part_routes: slot_index(part_routes, EXPERTS, CAP))(routes.reshape(sources, ROWS, TOPK))

    def fill(rows, slot):
        return jnp.zeros((EXPERTS * CAP, D), jnp.bfloat16).at[slot].set(jnp.repeat(rows, TOPK, axis=0))
    buffers = jax.vmap(fill)(src_rows, slots)
    per_expert = jnp.swapaxes(buffers.reshape(sources, EXPERTS, CAP, D), 0, 1).reshape(EXPERTS, sources * CAP, D)
    outputs = lax.map(expert_rows, (per_expert, w_gate, w_up, w_down))
    outputs = jnp.swapaxes(outputs.reshape(EXPERTS, sources, CAP, D), 0, 1).reshape(sources, EXPERTS * CAP, D)
    picked = jax.vmap(lambda rows, slot: rows[slot])(outputs, slots).reshape(TOKENS, TOPK, D)
    difference = pair_logits[:, 0] - pair_logits[:, 1]
    pair_weight = jnp.stack([jax.nn.sigmoid(difference), jax.nn.sigmoid(-difference)], axis=1)
    route_weight = group_prob[:, None] * pair_weight
    moe = lax.optimization_barrier(jnp.sum(route_weight[:, :, None] * picked.astype(jnp.float32), axis=1))
    return layer_norm(residual_scale * normed.astype(jnp.float32) + moe, gain_two, shift_two).astype(jnp.bfloat16)
```

```python
import functools

import jax
import jax.numpy as jnp
from jax import lax
from jax.experimental import pallas as pl
from jax.experimental.pallas import tpu as pltpu
from jax.sharding import PartitionSpec as P

HEAD_DIM = 128
GROUPS = 4
TOPK = 2
MESH = pl.DeviceIdType.MESH

residual_scale = 8.0**0.25
norm_eps = 1e-05


def remote(src, dst, send_sem, recv_sem, target):
    return pltpu.make_async_remote_copy(
        src_ref=src,
        dst_ref=dst,
        send_sem=send_sem,
        recv_sem=recv_sem,
        device_id=target,
        device_id_type=MESH,
    )


def norm_rows(rows, gain, shift):
    mean = jnp.mean(rows, axis=-1, keepdims=True)
    centred = rows - mean
    variance = jnp.mean(centred * centred, axis=-1, keepdims=True)
    return centred * lax.rsqrt(variance + norm_eps) * gain + shift


def attend_kernel(
    n_sp,
    n_tp,
    chunks,
    off_ref,
    q_ref,
    k_ref,
    v_ref,
    gain_ref,
    shift_ref,
    res_hbm,
    w_hbm,
    out_ref,
    kv,
    w_ref,
    res_ref,
    later_ref,
    carry,
    acc,
    att,
    send1,
    keep1,
    recv1,
    send2,
    recv2,
    rows_ref,
    load_sem,
    kv_send,
    kv_recv,
    s1,
    r1,
    s2,
    r2,
):
    me = lax.axis_index("sp")
    t = lax.axis_index("tp")
    rows = q_ref.shape[0]
    heads = q_ref.shape[1] // HEAD_DIM
    local = res_ref.shape[0]
    cols = w_ref.shape[1] // chunks
    near = t + 1 - 2 * lax.rem(t, 2)
    far = lax.rem(t + 2, 4)

    load_w = pltpu.make_async_copy(w_hbm, w_ref, load_sem.at[0])
    load_res = pltpu.make_async_copy(res_hbm, res_ref, load_sem.at[1])
    load_w.start()
    load_res.start()

    barrier = pltpu.get_barrier_semaphore()
    for step in (1, n_sp - 1):
        pl.semaphore_signal(
            barrier, inc=1, device_id={"sp": lax.rem(me + step, n_sp)}, device_id_type=MESH
        )
    for partner in (near, far):
        pl.semaphore_signal(barrier, inc=1, device_id={"tp": partner}, device_id_type=MESH)
    pl.semaphore_wait(barrier, 4)

    up = {"sp": lax.rem(me + 1, n_sp)}
    own = [
        remote(ref, kv.at[me, i], kv_send.at[me, i], kv_recv.at[me, i], up)
        for i, ref in enumerate((k_ref, v_ref))
    ]

    def passed(j, i):
        return remote(kv.at[j, i], kv.at[j, i], kv_send.at[j, i], kv_recv.at[j, i], up)

    @pl.when(me < n_sp - 1)
    def _():
        own[0].start()
        own[1].start()

    row_id = lax.broadcasted_iota(jnp.int32, (rows, rows), 0)
    col_id = lax.broadcasted_iota(jnp.int32, (rows, rows), 1)
    later_ref[...] = jnp.where(row_id > col_id, 1.0, 0.0).astype(jnp.bfloat16)
    scale = HEAD_DIM ** (-0.5)

    def block(key_of, value_of, first):
        for h in range(heads):
            span = slice(h * HEAD_DIM, (h + 1) * HEAD_DIM)
            score = (
                lax.dot_general(
                    q_ref[:, span],
                    key_of(span),
                    (((1,), (1,)), ((), ())),
                    preferred_element_type=jnp.float32,
                )
                * scale
                - off_ref[h]
            )
            soft = jnp.maximum(score, 0.0) + jnp.log(1.0 + jnp.exp(-jnp.abs(score)))
            gain = score - soft
            if first:
                soft = jnp.where(col_id < row_id, soft, 0.0)
            high = soft.astype(jnp.bfloat16)
            low = (soft - high.astype(jnp.float32)).astype(jnp.bfloat16)
            tail = jnp.dot(high, later_ref[...], preferred_element_type=jnp.float32)
            tail = tail + jnp.dot(low, later_ref[...], preferred_element_type=jnp.float32)
            total = jnp.sum(soft, axis=1, keepdims=True)
            if first:
                weight = jnp.where(col_id < row_id, jnp.exp(gain - tail), 0.0)
                carry[h] = total
            else:
                weight = jnp.exp(gain - tail - carry[h])
                carry[h] = carry[h] + total
            part = jnp.dot(
                weight.astype(jnp.bfloat16), value_of(span), preferred_element_type=jnp.float32
            )
            if first:
                acc[:, span] = part
            else:
                acc[:, span] = acc[:, span] + part

    block(lambda span: k_ref[:, span], lambda span: v_ref[:, span], True)

    def turn(step, _):
        j = me - step
        for i in range(2):
            passed(j, i).wait_recv()

            @pl.when(me < n_sp - 1)
            def _():
                passed(j, i).start()

        block(lambda span: kv[j, 0, :, span], lambda span: kv[j, 1, :, span], False)
        return 0

    lax.fori_loop(1, me + 1, turn, 0)

    att[...] = acc[...].astype(jnp.bfloat16)
    order = (
        near + 2 - 4 * (near // 2),
        near,
        far,
        t,
    )
    picked = jnp.concatenate(
        [att[pl.ds(pl.multiple_of(b * local, local), local), :] for b in order], axis=0
    )
    half = rows // 2
    load_w.wait()
    load_res.wait()

    def hop1(c):
        return remote(send1.at[c], recv1.at[c], s1.at[c], r1.at[c], {"tp": near})

    def hop2(c):
        return remote(send2.at[c], recv2.at[c], s2.at[c], r2.at[c], {"tp": far})

    for c in range(chunks):
        part = jnp.dot(
            picked, w_ref[:, c * cols : (c + 1) * cols], preferred_element_type=jnp.float32
        ).astype(jnp.bfloat16)
        send1[c] = part[:half]
        keep1[c] = part[half:]
        hop1(c).start()
    for c in range(chunks):
        hop1(c).wait_recv()
        both = keep1[c].astype(jnp.float32) + recv1[c].astype(jnp.float32)
        send2[c] = both[:local].astype(jnp.bfloat16)
        hop2(c).start()
        span = slice(c * cols, (c + 1) * cols)
        rows_ref[:, span] = (
            residual_scale * res_ref[:, span].astype(jnp.float32) + both[local:]
        )
    for c in range(chunks):
        hop2(c).wait_recv()
        span = slice(c * cols, (c + 1) * cols)
        rows_ref[:, span] = rows_ref[:, span] + recv2[c].astype(jnp.float32)
    out_ref[...] = norm_rows(rows_ref[...], gain_ref[...], shift_ref[...]).astype(jnp.bfloat16)

    for c in range(chunks):
        hop1(c).wait_send()
        hop2(c).wait_send()

    @pl.when(me < n_sp - 1)
    def _():
        own[0].wait_send()
        own[1].wait_send()

        def drain(step, _):
            for i in range(2):
                passed(me - step, i).wait_send()
            return 0

        lax.fori_loop(1, me + 1, drain, 0)


def attend(queries, keys, values, offsets, residual, out_weight, gain, shift):
    n_sp, n_tp = lax.axis_size("sp"), lax.axis_size("tp")
    assert n_tp == 4
    rows, inner = queries.shape
    local, width = residual.shape
    heads = offsets.shape[0]
    chunks = 8
    cols = width // chunks
    half = rows // 2
    vmem = pl.BlockSpec(memory_space=pltpu.VMEM)
    hbm = pl.BlockSpec(memory_space=pl.ANY)
    dma = pltpu.SemaphoreType.DMA
    bf16, f32 = jnp.bfloat16, jnp.float32
    return pl.pallas_call(
        functools.partial(attend_kernel, n_sp, n_tp, chunks),
        out_shape=jax.ShapeDtypeStruct((local, width), bf16),
        in_specs=[pl.BlockSpec(memory_space=pltpu.SMEM), vmem, vmem, vmem, vmem, vmem, hbm, hbm],
        out_specs=vmem,
        scratch_shapes=[
            pltpu.VMEM((n_sp, 2, rows, inner), bf16),
            pltpu.VMEM(out_weight.shape, bf16),
            pltpu.VMEM(residual.shape, bf16),
            pltpu.VMEM((rows, rows), bf16),
            pltpu.VMEM((heads, rows, 1), f32),
            pltpu.VMEM((rows, inner), f32),
            pltpu.VMEM((rows, inner), bf16),
            pltpu.VMEM((chunks, half, cols), bf16),
            pltpu.VMEM((chunks, half, cols), bf16),
            pltpu.VMEM((chunks, half, cols), bf16),
            pltpu.VMEM((chunks, local, cols), bf16),
            pltpu.VMEM((chunks, local, cols), bf16),
            pltpu.VMEM((local, width), f32),
            dma((2,)),
            dma((n_sp, 2)),
            dma((n_sp, 2)),
            dma((chunks,)),
            dma((chunks,)),
            dma((chunks,)),
            dma((chunks,)),
        ],
        compiler_params=pltpu.CompilerParams(collective_id=0, has_side_effects=True),
        name="attend",
    )(offsets, queries, keys, values, gain[None], shift[None], residual, out_weight)


def layer_norm(rows, gain, shift):
    mean = jnp.mean(rows, axis=-1, keepdims=True)
    centred = rows - mean
    variance = jnp.mean(centred * centred, axis=-1, keepdims=True)
    return centred * lax.rsqrt(variance + norm_eps) * gain + shift


def slot_index(routes, expert_count, capacity):
    flat = routes.reshape(-1)
    onehot = (flat[:, None] == jnp.arange(expert_count, dtype=jnp.int32)[None, :]).astype(jnp.int32)
    earlier = jnp.cumsum(onehot, axis=0) - onehot
    rank = jnp.sum(earlier * onehot, axis=1)
    return flat * capacity + rank


def expert_rows(rows, gate_w, up_w, down_w):
    gate = jnp.dot(rows, gate_w, preferred_element_type=jnp.float32)
    upper = jnp.dot(rows, up_w, preferred_element_type=jnp.float32)
    hidden = (jax.nn.silu(gate) * upper).astype(jnp.bfloat16)
    return jnp.dot(hidden, down_w, preferred_element_type=jnp.float32).astype(jnp.bfloat16)


def per_device(
    queries,
    keys,
    values,
    offsets,
    residual,
    out_weight,
    gain_one,
    shift_one,
    gain_two,
    shift_two,
    group_prob,
    pair_logits,
    routes,
    w_gate,
    w_up,
    w_down,
):
    normed = attend(
        queries, keys, values, offsets, residual, out_weight, gain_one, shift_one
    )
    local_rows = residual.shape[0]
    width = normed.shape[1]
    expert_count = lax.axis_size("sp") * lax.axis_size("tp")
    capacity = local_rows // (expert_count // GROUPS)
    slots = slot_index(routes, expert_count, capacity)
    buffer = (
        jnp.zeros((expert_count * capacity, width), jnp.bfloat16)
        .at[slots]
        .set(jnp.repeat(normed, TOPK, axis=0))
    )
    arrived = lax.all_to_all(
        buffer.reshape(expert_count, capacity, width),
        ("sp", "tp"),
        split_axis=0,
        concat_axis=0,
        tiled=True,
    )
    result = expert_rows(arrived.reshape(-1, width), w_gate[0], w_up[0], w_down[0]).reshape(
        expert_count, capacity, width
    )
    returned = lax.all_to_all(result, ("sp", "tp"), split_axis=0, concat_axis=0, tiled=True)
    picked = returned.reshape(-1, width)[slots].reshape(local_rows, TOPK, width)
    difference = pair_logits[:, 0] - pair_logits[:, 1]
    pair_weight = jnp.stack([jax.nn.sigmoid(difference), jax.nn.sigmoid(-difference)], axis=1)
    route_weight = group_prob[:, None] * pair_weight
    moe = jnp.sum(route_weight[:, :, None] * picked.astype(jnp.float32), axis=1)
    return layer_norm(
        residual_scale * normed.astype(jnp.float32) + moe, gain_two, shift_two
    ).astype(jnp.bfloat16)


def solution(mesh):
    return jax.shard_map(
        per_device,
        mesh=mesh,
        in_specs=(
            P(("grp", "sp"), "tp"),
            P(("grp", "sp"), "tp"),
            P(("grp", "sp"), "tp"),
            P("tp"),
            P(("grp", "sp", "tp"), None),
            P("tp", None),
            P(),
            P(),
            P(),
            P(),
            P(("grp", "sp", "tp")),
            P(("grp", "sp", "tp"), None),
            P(("grp", "sp", "tp"), None),
            P(("sp", "tp"), None, None),
            P(("sp", "tp"), None, None),
            P(("sp", "tp"), None, None),
        ),
        out_specs=P(("grp", "sp", "tp"), None),
        check_vma=False,
    )
```

```python
import functools

import jax
import jax.numpy as jnp
from jax import lax
from jax.experimental import pallas as pl
from jax.experimental.pallas import tpu as pltpu
from jax.sharding import PartitionSpec as P

HEAD_DIM = 128
GROUPS = 4
TOPK = 2
MESH = pl.DeviceIdType.MESH

residual_scale = 8.0**0.25
norm_eps = 1e-05


def remote(src, dst, send_sem, recv_sem, target):
    return pltpu.make_async_remote_copy(
        src_ref=src,
        dst_ref=dst,
        send_sem=send_sem,
        recv_sem=recv_sem,
        device_id=target,
        device_id_type=MESH,
    )


def norm_rows(rows, gain, shift):
    mean = jnp.mean(rows, axis=-1, keepdims=True)
    centred = rows - mean
    variance = jnp.mean(centred * centred, axis=-1, keepdims=True)
    return centred * lax.rsqrt(variance + norm_eps) * gain + shift


def attend_kernel(
    n_sp,
    n_tp,
    chunks,
    off_ref,
    q_ref,
    k_ref,
    v_ref,
    gain_ref,
    shift_ref,
    res_hbm,
    w_hbm,
    out_ref,
    kv,
    w_ref,
    res_ref,
    later_ref,
    carry,
    acc,
    att,
    send1,
    keep1,
    recv1,
    send2,
    recv2,
    rows_ref,
    load_sem,
    kv_send,
    kv_recv,
    s1,
    r1,
    s2,
    r2,
):
    me = lax.axis_index("sp")
    t = lax.axis_index("tp")
    rows = q_ref.shape[0]
    heads = q_ref.shape[1] // HEAD_DIM
    local = res_ref.shape[0]
    cols = w_ref.shape[1] // chunks
    near = t + 1 - 2 * lax.rem(t, 2)
    far = lax.rem(t + 2, 4)

    load_w = pltpu.make_async_copy(w_hbm, w_ref, load_sem.at[0])
    load_res = pltpu.make_async_copy(res_hbm, res_ref, load_sem.at[1])
    load_w.start()
    load_res.start()

    barrier = pltpu.get_barrier_semaphore()
    for step in (1, n_sp - 1):
        pl.semaphore_signal(
            barrier, inc=1, device_id={"sp": lax.rem(me + step, n_sp)}, device_id_type=MESH
        )
    for partner in (near, far):
        pl.semaphore_signal(barrier, inc=1, device_id={"tp": partner}, device_id_type=MESH)
    pl.semaphore_wait(barrier, 4)

    up = {"sp": lax.rem(me + 1, n_sp)}
    own = [
        remote(ref, kv.at[me, i], kv_send.at[me, i], kv_recv.at[me, i], up)
        for i, ref in enumerate((k_ref, v_ref))
    ]

    def passed(j, i):
        return remote(kv.at[j, i], kv.at[j, i], kv_send.at[j, i], kv_recv.at[j, i], up)

    @pl.when(me < n_sp - 1)
    def _():
        own[0].start()
        own[1].start()

    row_id = lax.broadcasted_iota(jnp.int32, (rows, rows), 0)
    col_id = lax.broadcasted_iota(jnp.int32, (rows, rows), 1)
    later_ref[...] = jnp.where(row_id > col_id, 1.0, 0.0).astype(jnp.bfloat16)
    scale = HEAD_DIM ** (-0.5)

    def block(key_of, value_of, first):
        for h in range(heads):
            span = slice(h * HEAD_DIM, (h + 1) * HEAD_DIM)
            score = (
                lax.dot_general(
                    q_ref[:, span],
                    key_of(span),
                    (((1,), (1,)), ((), ())),
                    preferred_element_type=jnp.float32,
                )
                * scale
                - off_ref[h]
            )
            soft = jnp.maximum(score, 0.0) + jnp.log(1.0 + jnp.exp(-jnp.abs(score)))
            gain = score - soft
            if first:
                soft = jnp.where(col_id < row_id, soft, 0.0)
            high = soft.astype(jnp.bfloat16)
            low = (soft - high.astype(jnp.float32)).astype(jnp.bfloat16)
            tail = jnp.dot(high, later_ref[...], preferred_element_type=jnp.float32)
            tail = tail + jnp.dot(low, later_ref[...], preferred_element_type=jnp.float32)
            total = jnp.sum(soft, axis=1, keepdims=True)
            if first:
                weight = jnp.where(col_id < row_id, jnp.exp(gain - tail), 0.0)
                carry[h] = total
            else:
                weight = jnp.exp(gain - tail - carry[h])
                carry[h] = carry[h] + total
            part = jnp.dot(
                weight.astype(jnp.bfloat16), value_of(span), preferred_element_type=jnp.float32
            )
            if first:
                acc[:, span] = part
            else:
                acc[:, span] = acc[:, span] + part

    block(lambda span: k_ref[:, span], lambda span: v_ref[:, span], True)

    def turn(step, _):
        j = me - step
        for i in range(2):
            passed(j, i).wait_recv()

            @pl.when(me < n_sp - 1)
            def _():
                passed(j, i).start()

        block(lambda span: kv[j, 0, :, span], lambda span: kv[j, 1, :, span], False)
        return 0

    lax.fori_loop(1, me + 1, turn, 0)

    att[...] = acc[...].astype(jnp.bfloat16)
    order = (
        near + 2 - 4 * (near // 2),
        near,
        far,
        t,
    )
    picked = jnp.concatenate(
        [att[pl.ds(pl.multiple_of(b * local, local), local), :] for b in order], axis=0
    )
    half = rows // 2
    load_w.wait()
    load_res.wait()

    def hop1(c):
        return remote(send1.at[c], recv1.at[c], s1.at[c], r1.at[c], {"tp": near})

    def hop2(c):
        return remote(send2.at[c], recv2.at[c], s2.at[c], r2.at[c], {"tp": far})

    for c in range(chunks):
        part = jnp.dot(
            picked, w_ref[:, c * cols : (c + 1) * cols], preferred_element_type=jnp.float32
        ).astype(jnp.bfloat16)
        send1[c] = part[:half]
        keep1[c] = part[half:]
        hop1(c).start()
    for c in range(chunks):
        hop1(c).wait_recv()
        both = keep1[c].astype(jnp.float32) + recv1[c].astype(jnp.float32)
        send2[c] = both[:local].astype(jnp.bfloat16)
        hop2(c).start()
        span = slice(c * cols, (c + 1) * cols)
        rows_ref[:, span] = (
            residual_scale * res_ref[:, span].astype(jnp.float32) + both[local:]
        )
    for c in range(chunks):
        hop2(c).wait_recv()
        span = slice(c * cols, (c + 1) * cols)
        rows_ref[:, span] = rows_ref[:, span] + recv2[c].astype(jnp.float32)
    out_ref[...] = norm_rows(rows_ref[...], gain_ref[...], shift_ref[...]).astype(jnp.bfloat16)

    for c in range(chunks):
        hop1(c).wait_send()
        hop2(c).wait_send()

    @pl.when(me < n_sp - 1)
    def _():
        own[0].wait_send()
        own[1].wait_send()

        def drain(step, _):
            for i in range(2):
                passed(me - step, i).wait_send()
            return 0

        lax.fori_loop(1, me + 1, drain, 0)


def attend(queries, keys, values, offsets, residual, out_weight, gain, shift):
    n_sp, n_tp = lax.axis_size("sp"), lax.axis_size("tp")
    assert n_tp == 4
    rows, inner = queries.shape
    local, width = residual.shape
    heads = offsets.shape[0]
    chunks = 8
    cols = width // chunks
    half = rows // 2
    vmem = pl.BlockSpec(memory_space=pltpu.VMEM)
    hbm = pl.BlockSpec(memory_space=pl.ANY)
    dma = pltpu.SemaphoreType.DMA
    bf16, f32 = jnp.bfloat16, jnp.float32
    return pl.pallas_call(
        functools.partial(attend_kernel, n_sp, n_tp, chunks),
        out_shape=jax.ShapeDtypeStruct((local, width), bf16),
        in_specs=[pl.BlockSpec(memory_space=pltpu.SMEM), vmem, vmem, vmem, vmem, vmem, hbm, hbm],
        out_specs=vmem,
        scratch_shapes=[
            pltpu.VMEM((n_sp, 2, rows, inner), bf16),
            pltpu.VMEM(out_weight.shape, bf16),
            pltpu.VMEM(residual.shape, bf16),
            pltpu.VMEM((rows, rows), bf16),
            pltpu.VMEM((heads, rows, 1), f32),
            pltpu.VMEM((rows, inner), f32),
            pltpu.VMEM((rows, inner), bf16),
            pltpu.VMEM((chunks, half, cols), bf16),
            pltpu.VMEM((chunks, half, cols), bf16),
            pltpu.VMEM((chunks, half, cols), bf16),
            pltpu.VMEM((chunks, local, cols), bf16),
            pltpu.VMEM((chunks, local, cols), bf16),
            pltpu.VMEM((local, width), f32),
            dma((2,)),
            dma((n_sp, 2)),
            dma((n_sp, 2)),
            dma((chunks,)),
            dma((chunks,)),
            dma((chunks,)),
            dma((chunks,)),
        ],
        compiler_params=pltpu.CompilerParams(collective_id=0, has_side_effects=True),
        name="attend",
    )(offsets, queries, keys, values, gain[None], shift[None], residual, out_weight)


def experts_kernel(
    n_sp,
    n_tp,
    slots,
    extra,
    x_ref,
    routes_ref,
    prob_ref,
    logit_ref,
    gain_ref,
    shift_ref,
    gate_hbm,
    up_hbm,
    down_hbm,
    out_ref,
    w_in,
    w_out,
    place,
    outbox,
    inbox,
    partial,
    near_in,
    far_out,
    far_in,
    done,
    returned,
    rows_ref,
    load_sem,
    zs,
    zr,
    fs,
    fr,
    ns,
    nr,
    ps,
    pr,
    qs,
    qr,
    bs,
    br,
):
    me = lax.axis_index("sp")
    t = lax.axis_index("tp")
    near = t + 1 - 2 * lax.rem(t, 2)
    far = lax.rem(t + 2, 4)
    across = lax.rem(near + 2, 4)
    local, width = x_ref.shape
    hidden_width = w_out.shape[0]
    count = n_sp * n_tp
    f32, bf16 = jnp.float32, jnp.bfloat16
    step_cols = 1024 if width % 1024 == 0 else width

    loads = [
        pltpu.make_async_copy(gate_hbm.at[0], w_in.at[:, :hidden_width], load_sem.at[0]),
        pltpu.make_async_copy(up_hbm.at[0], w_in.at[:, hidden_width:], load_sem.at[1]),
        pltpu.make_async_copy(down_hbm.at[0], w_out, load_sem.at[2]),
    ]
    for load in loads:
        load.start()

    barrier = pltpu.get_barrier_semaphore()
    for step in range(1, n_sp):
        pl.semaphore_signal(
            barrier, inc=1, device_id={"sp": lax.rem(me + step, n_sp)}, device_id_type=MESH
        )
    for partner in (near, far):
        pl.semaphore_signal(barrier, inc=1, device_id={"tp": partner}, device_id_type=MESH)

    first, second = routes_ref[:, 0:1], routes_ref[:, 1:2]
    line = lax.broadcasted_iota(jnp.int32, (local, n_sp), 1)
    member = jnp.where(
        (line == first // n_tp) | (line == second // n_tp), 1.0, 0.0
    ).astype(bf16)
    before = jnp.where(
        lax.broadcasted_iota(jnp.int32, (local, local), 1)
        < lax.broadcasted_iota(jnp.int32, (local, local), 0),
        1.0,
        0.0,
    ).astype(bf16)
    rank = jnp.dot(before, member, preferred_element_type=f32).astype(bf16)
    total = n_sp * slots
    spread = jnp.where(
        lax.broadcasted_iota(jnp.int32, (n_sp, total), 1) // slots
        == lax.broadcasted_iota(jnp.int32, (n_sp, total), 0),
        1.0,
        0.0,
    ).astype(bf16)
    member_wide = jnp.dot(member, spread, preferred_element_type=f32)
    rank_wide = jnp.dot(rank, spread, preferred_element_type=f32)
    slot_id = lax.rem(lax.broadcasted_iota(jnp.int32, (local, total), 1), slots).astype(f32)
    place[...] = jnp.where((member_wide > 0.5) & (rank_wide == slot_id), 1.0, 0.0).astype(bf16)

    difference = logit_ref[:, 0:1] - logit_ref[:, 1:2]
    weight_one = prob_ref[...] / (1.0 + jnp.exp(-difference))
    weight_two = prob_ref[...] / (1.0 + jnp.exp(difference))
    lane = lax.broadcasted_iota(jnp.int32, (local, extra), 1)
    name = lax.rem(lane, count)
    value = jnp.where(name == first, weight_one, 0.0) + jnp.where(name == second, weight_two, 0.0)
    value = jnp.where(lane < 2 * count, value, 0.0)
    high = value.astype(bf16)
    low = (value - high.astype(f32)).astype(bf16)
    tags = jnp.where(lane < count, high.astype(f32), low.astype(f32)).astype(bf16)

    def placed(rows):
        return lax.dot_general(
            place[...], rows, (((0,), (0,)), ((), ())), preferred_element_type=f32
        ).astype(bf16)

    for c in range(0, width, step_cols):
        outbox[:, :, c : c + step_cols] = placed(x_ref[:, c : c + step_cols]).reshape(
            n_sp, slots, step_cols
        )
    outbox[:, :, width:] = placed(tags).reshape(n_sp, slots, extra)

    pl.semaphore_wait(barrier, n_sp + 1)

    def go(z):
        return remote(outbox.at[z], inbox.at[me, t], zs.at[z], zr.at[me], {"sp": z})

    def come(z):
        return remote(outbox.at[z], inbox.at[z, t], zs.at[z], zr.at[z], {"sp": z})

    def to_far(z):
        return remote(inbox.at[z, t], inbox.at[z, t], fs.at[z], fr.at[z], {"tp": far})

    def to_near(z, i):
        block = inbox.at[z, (t, far)[i]]
        return remote(block, block, ns.at[z, i], nr.at[z, i], {"tp": near})

    def part_near(z, i):
        return remote(
            partial.at[z, (near, across)[i]],
            near_in.at[z, i],
            ps.at[z, i],
            pr.at[z, i],
            {"tp": near},
        )

    def part_far(z):
        return remote(far_out.at[z], far_in.at[z], qs.at[z], qr.at[z], {"tp": far})

    def back(z):
        return remote(done.at[z], returned.at[me], bs.at[z], br.at[me], {"sp": z})

    def back_in(z):
        return remote(done.at[z], returned.at[z], bs.at[z], br.at[z], {"sp": z})

    def send_out(step, _):
        go(lax.rem(me + step, n_sp)).start()
        return 0

    lax.fori_loop(1, n_sp, send_out, 0)
    inbox[me, t] = outbox[me]

    def run_experts(z):
        rows = inbox[z].reshape(n_tp * slots, width + extra)
        own = me * n_tp + t
        tag = rows[:, width:].astype(f32)
        tag_lane = lax.broadcasted_iota(jnp.int32, tag.shape, 1)
        weight = jnp.sum(
            jnp.where((tag_lane == own) | (tag_lane == own + count), tag, 0.0),
            axis=1,
            keepdims=True,
        )
        both = jnp.dot(rows[:, :width], w_in[...], preferred_element_type=f32)
        gate, upper = both[:, :hidden_width], both[:, hidden_width:]
        hidden = (gate / (1.0 + jnp.exp(-gate)) * upper).astype(bf16)
        for c in range(0, width, step_cols):
            part = jnp.dot(
                hidden, w_out[:, c : c + step_cols], preferred_element_type=f32
            ).astype(bf16)
            partial[z, :, :, c : c + step_cols] = (
                (part.astype(f32) * weight).astype(bf16).reshape(n_tp, slots, step_cols)
            )

    def turn(step, _):
        @pl.when(step < n_sp)
        def _():
            z = lax.rem(me - step + n_sp, n_sp)

            @pl.when(step > 0)
            def _():
                come(z).wait_recv()

            to_far(z).start()
            to_near(z, 0).start()

        @pl.when(step == 1)
        def _():
            for load in loads:
                load.wait()

        @pl.when((step >= 1) & (step <= n_sp))
        def _():
            z = lax.rem(me - step + 1 + n_sp, n_sp)
            to_far(z).wait_recv()
            to_near(z, 1).start()
            to_near(z, 0).wait_recv()
            to_near(z, 1).wait_recv()
            run_experts(z)
            part_near(z, 1).start()
            part_near(z, 0).start()
            part_near(z, 1).wait_recv()
            far_out[z] = (partial[z, far].astype(f32) + near_in[z, 1].astype(f32)).astype(bf16)
            part_far(z).start()
            part_near(z, 0).wait_recv()

        @pl.when(step >= 2)
        def _():
            z = lax.rem(me - step + 2 + n_sp, n_sp)
            part_far(z).wait_recv()
            whole = (
                partial[z, t].astype(f32) + near_in[z, 0].astype(f32) + far_in[z].astype(f32)
            ).astype(bf16)

            @pl.when(z == me)
            def _():
                returned[me] = whole

            @pl.when(z != me)
            def _():
                done[z] = whole
                back(z).start()

        return 0

    lax.fori_loop(0, n_sp + 2, turn, 0)

    def collect(step, _):
        back_in(lax.rem(me + step, n_sp)).wait_recv()
        return 0

    lax.fori_loop(1, n_sp, collect, 0)
    for c in range(0, width, step_cols):
        span = slice(c, c + step_cols)
        moe = jnp.dot(
            place[...], returned[:, :, span].reshape(total, step_cols), preferred_element_type=f32
        )
        rows_ref[:, span] = residual_scale * x_ref[:, span].astype(f32) + moe
    out_ref[...] = norm_rows(rows_ref[...], gain_ref[...], shift_ref[...]).astype(bf16)

    def drain(step, _):
        z = lax.rem(me + step, n_sp)

        @pl.when(step > 0)
        def _():
            go(z).wait_send()
            back(z).wait_send()

        to_far(z).wait_send()
        part_far(z).wait_send()
        for i in range(2):
            to_near(z, i).wait_send()
            part_near(z, i).wait_send()
        return 0

    lax.fori_loop(0, n_sp, drain, 0)


def experts(normed, routes, group_prob, pair_logits, gain, shift, w_gate, w_up, w_down):
    n_sp, n_tp = lax.axis_size("sp"), lax.axis_size("tp")
    assert n_tp == 4
    local, width = normed.shape
    hidden = w_down.shape[1]
    count = n_sp * n_tp
    group = count // GROUPS
    capacity = local // group
    slots = n_tp * capacity
    if n_tp % group == 0:
        slots = slots // TOPK
    extra = -(-2 * count // 128) * 128
    vmem = pl.BlockSpec(memory_space=pltpu.VMEM)
    hbm = pl.BlockSpec(memory_space=pl.ANY)
    dma = pltpu.SemaphoreType.DMA
    bf16, f32 = jnp.bfloat16, jnp.float32
    return pl.pallas_call(
        functools.partial(experts_kernel, n_sp, n_tp, slots, extra),
        out_shape=jax.ShapeDtypeStruct((local, width), bf16),
        in_specs=[vmem] * 6 + [hbm] * 3,
        out_specs=vmem,
        scratch_shapes=[
            pltpu.VMEM((width, 2 * hidden), bf16),
            pltpu.VMEM((hidden, width), bf16),
            pltpu.VMEM((local, n_sp * slots), bf16),
            pltpu.VMEM((n_sp, slots, width + extra), bf16),
            pltpu.VMEM((n_sp, n_tp, slots, width + extra), bf16),
            pltpu.VMEM((n_sp, n_tp, slots, width), bf16),
            pltpu.VMEM((n_sp, 2, slots, width), bf16),
            pltpu.VMEM((n_sp, slots, width), bf16),
            pltpu.VMEM((n_sp, slots, width), bf16),
            pltpu.VMEM((n_sp, slots, width), bf16),
            pltpu.VMEM((n_sp, slots, width), bf16),
            pltpu.VMEM((local, width), f32),
            dma((3,)),
            dma((n_sp,)),
            dma((n_sp,)),
            dma((n_sp,)),
            dma((n_sp,)),
            dma((n_sp, 2)),
            dma((n_sp, 2)),
            dma((n_sp, 2)),
            dma((n_sp, 2)),
            dma((n_sp,)),
            dma((n_sp,)),
            dma((n_sp,)),
            dma((n_sp,)),
        ],
        compiler_params=pltpu.CompilerParams(collective_id=1, has_side_effects=True),
        name="experts",
    )(
        normed,
        routes,
        group_prob[:, None],
        pair_logits,
        gain[None],
        shift[None],
        w_gate,
        w_up,
        w_down,
    )


def per_device(
    queries,
    keys,
    values,
    offsets,
    residual,
    out_weight,
    gain_one,
    shift_one,
    gain_two,
    shift_two,
    group_prob,
    pair_logits,
    routes,
    w_gate,
    w_up,
    w_down,
):
    normed = attend(
        queries, keys, values, offsets, residual, out_weight, gain_one, shift_one
    )
    return experts(
        normed, routes, group_prob, pair_logits, gain_two, shift_two, w_gate, w_up, w_down
    )


def solution(mesh):
    return jax.shard_map(
        per_device,
        mesh=mesh,
        in_specs=(
            P(("grp", "sp"), "tp"),
            P(("grp", "sp"), "tp"),
            P(("grp", "sp"), "tp"),
            P("tp"),
            P(("grp", "sp", "tp"), None),
            P("tp", None),
            P(),
            P(),
            P(),
            P(),
            P(("grp", "sp", "tp")),
            P(("grp", "sp", "tp"), None),
            P(("grp", "sp", "tp"), None),
            P(("sp", "tp"), None, None),
            P(("sp", "tp"), None, None),
            P(("sp", "tp"), None, None),
        ),
        out_specs=P(("grp", "sp", "tp"), None),
        check_vma=False,
    )
```

```python
import functools

import jax
import jax.numpy as jnp
from jax import lax
from jax.experimental import pallas as pl
from jax.experimental.pallas import tpu as pltpu
from jax.sharding import PartitionSpec as P

HEAD_DIM = 128
GROUPS = 4
TOPK = 2
MESH = pl.DeviceIdType.MESH

residual_scale = 8.0**0.25
norm_eps = 1e-05


def remote(src, dst, send_sem, recv_sem, target):
    return pltpu.make_async_remote_copy(
        src_ref=src,
        dst_ref=dst,
        send_sem=send_sem,
        recv_sem=recv_sem,
        device_id=target,
        device_id_type=MESH,
    )


def norm_rows(rows, gain, shift):
    mean = jnp.mean(rows, axis=-1, keepdims=True)
    centred = rows - mean
    variance = jnp.mean(centred * centred, axis=-1, keepdims=True)
    return centred * lax.rsqrt(variance + norm_eps) * gain + shift


def attend_kernel(
    n_sp,
    n_tp,
    chunks,
    off_ref,
    q_ref,
    k_ref,
    v_ref,
    gain_ref,
    shift_ref,
    res_hbm,
    w_hbm,
    out_ref,
    kv,
    w_ref,
    res_ref,
    later_ref,
    carry,
    acc,
    att,
    send1,
    keep1,
    recv1,
    send2,
    recv2,
    rows_ref,
    load_sem,
    kv_send,
    kv_recv,
    s1,
    r1,
    s2,
    r2,
):
    me = lax.axis_index("sp")
    t = lax.axis_index("tp")
    rows = q_ref.shape[0]
    heads = q_ref.shape[1] // HEAD_DIM
    local = res_ref.shape[0]
    cols = w_ref.shape[1] // chunks
    near = t + 1 - 2 * lax.rem(t, 2)
    far = lax.rem(t + 2, 4)

    load_w = pltpu.make_async_copy(w_hbm, w_ref, load_sem.at[0])
    load_res = pltpu.make_async_copy(res_hbm, res_ref, load_sem.at[1])
    load_w.start()
    load_res.start()

    barrier = pltpu.get_barrier_semaphore()
    for step in (1, n_sp - 1):
        pl.semaphore_signal(
            barrier, inc=1, device_id={"sp": lax.rem(me + step, n_sp)}, device_id_type=MESH
        )
    for partner in (near, far):
        pl.semaphore_signal(barrier, inc=1, device_id={"tp": partner}, device_id_type=MESH)
    pl.semaphore_wait(barrier, 4)

    up = {"sp": lax.rem(me + 1, n_sp)}
    own = [
        remote(ref, kv.at[me, i], kv_send.at[me, i], kv_recv.at[me, i], up)
        for i, ref in enumerate((k_ref, v_ref))
    ]

    def passed(j, i):
        return remote(kv.at[j, i], kv.at[j, i], kv_send.at[j, i], kv_recv.at[j, i], up)

    @pl.when(me < n_sp - 1)
    def _():
        own[0].start()
        own[1].start()

    row_id = lax.broadcasted_iota(jnp.int32, (rows, rows), 0)
    col_id = lax.broadcasted_iota(jnp.int32, (rows, rows), 1)
    later_ref[...] = jnp.where(row_id > col_id, 1.0, 0.0).astype(jnp.bfloat16)
    scale = HEAD_DIM ** (-0.5)

    def block(key_of, value_of, first):
        for h in range(heads):
            span = slice(h * HEAD_DIM, (h + 1) * HEAD_DIM)
            score = (
                lax.dot_general(
                    q_ref[:, span],
                    key_of(span),
                    (((1,), (1,)), ((), ())),
                    preferred_element_type=jnp.float32,
                )
                * scale
                - off_ref[h]
            )
            soft = jnp.maximum(score, 0.0) + jnp.log(1.0 + jnp.exp(-jnp.abs(score)))
            gain = score - soft
            if first:
                soft = jnp.where(col_id < row_id, soft, 0.0)
            high = soft.astype(jnp.bfloat16)
            low = (soft - high.astype(jnp.float32)).astype(jnp.bfloat16)
            tail = jnp.dot(high, later_ref[...], preferred_element_type=jnp.float32)
            tail = tail + jnp.dot(low, later_ref[...], preferred_element_type=jnp.float32)
            total = jnp.sum(soft, axis=1, keepdims=True)
            if first:
                weight = jnp.where(col_id < row_id, jnp.exp(gain - tail), 0.0)
                carry[h] = total
            else:
                weight = jnp.exp(gain - tail - carry[h])
                carry[h] = carry[h] + total
            part = jnp.dot(
                weight.astype(jnp.bfloat16), value_of(span), preferred_element_type=jnp.float32
            )
            if first:
                acc[:, span] = part
            else:
                acc[:, span] = acc[:, span] + part

    block(lambda span: k_ref[:, span], lambda span: v_ref[:, span], True)

    def turn(step, _):
        j = me - step
        for i in range(2):
            passed(j, i).wait_recv()

            @pl.when(me < n_sp - 1)
            def _():
                passed(j, i).start()

        block(lambda span: kv[j, 0, :, span], lambda span: kv[j, 1, :, span], False)
        return 0

    lax.fori_loop(1, me + 1, turn, 0)

    att[...] = acc[...].astype(jnp.bfloat16)
    order = (
        near + 2 - 4 * (near // 2),
        near,
        far,
        t,
    )
    picked = jnp.concatenate(
        [att[pl.ds(pl.multiple_of(b * local, local), local), :] for b in order], axis=0
    )
    half = rows // 2
    load_w.wait()
    load_res.wait()

    def hop1(c):
        return remote(send1.at[c], recv1.at[c], s1.at[c], r1.at[c], {"tp": near})

    def hop2(c):
        return remote(send2.at[c], recv2.at[c], s2.at[c], r2.at[c], {"tp": far})

    for c in range(chunks):
        part = jnp.dot(
            picked, w_ref[:, c * cols : (c + 1) * cols], preferred_element_type=jnp.float32
        ).astype(jnp.bfloat16)
        send1[c] = part[:half]
        keep1[c] = part[half:]
        hop1(c).start()
    for c in range(chunks):
        hop1(c).wait_recv()
        both = keep1[c].astype(jnp.float32) + recv1[c].astype(jnp.float32)
        send2[c] = both[:local].astype(jnp.bfloat16)
        hop2(c).start()
        span = slice(c * cols, (c + 1) * cols)
        rows_ref[:, span] = (
            residual_scale * res_ref[:, span].astype(jnp.float32) + both[local:]
        )
    for c in range(chunks):
        hop2(c).wait_recv()
        span = slice(c * cols, (c + 1) * cols)
        rows_ref[:, span] = rows_ref[:, span] + recv2[c].astype(jnp.float32)
    out_ref[...] = norm_rows(rows_ref[...], gain_ref[...], shift_ref[...]).astype(jnp.bfloat16)

    for c in range(chunks):
        hop1(c).wait_send()
        hop2(c).wait_send()

    @pl.when(me < n_sp - 1)
    def _():
        own[0].wait_send()
        own[1].wait_send()

        def drain(step, _):
            for i in range(2):
                passed(me - step, i).wait_send()
            return 0

        lax.fori_loop(1, me + 1, drain, 0)


def attend(queries, keys, values, offsets, residual, out_weight, gain, shift):
    n_sp, n_tp = lax.axis_size("sp"), lax.axis_size("tp")
    assert n_tp == 4
    rows, inner = queries.shape
    local, width = residual.shape
    heads = offsets.shape[0]
    chunks = 8
    cols = width // chunks
    half = rows // 2
    vmem = pl.BlockSpec(memory_space=pltpu.VMEM)
    hbm = pl.BlockSpec(memory_space=pl.ANY)
    dma = pltpu.SemaphoreType.DMA
    bf16, f32 = jnp.bfloat16, jnp.float32
    return pl.pallas_call(
        functools.partial(attend_kernel, n_sp, n_tp, chunks),
        out_shape=jax.ShapeDtypeStruct((local, width), bf16),
        in_specs=[pl.BlockSpec(memory_space=pltpu.SMEM), vmem, vmem, vmem, vmem, vmem, hbm, hbm],
        out_specs=vmem,
        scratch_shapes=[
            pltpu.VMEM((n_sp, 2, rows, inner), bf16),
            pltpu.VMEM(out_weight.shape, bf16),
            pltpu.VMEM(residual.shape, bf16),
            pltpu.VMEM((rows, rows), bf16),
            pltpu.VMEM((heads, rows, 1), f32),
            pltpu.VMEM((rows, inner), f32),
            pltpu.VMEM((rows, inner), bf16),
            pltpu.VMEM((chunks, half, cols), bf16),
            pltpu.VMEM((chunks, half, cols), bf16),
            pltpu.VMEM((chunks, half, cols), bf16),
            pltpu.VMEM((chunks, local, cols), bf16),
            pltpu.VMEM((chunks, local, cols), bf16),
            pltpu.VMEM((local, width), f32),
            dma((2,)),
            dma((n_sp, 2)),
            dma((n_sp, 2)),
            dma((chunks,)),
            dma((chunks,)),
            dma((chunks,)),
            dma((chunks,)),
        ],
        compiler_params=pltpu.CompilerParams(collective_id=0, has_side_effects=True),
        name="attend",
    )(offsets, queries, keys, values, gain[None], shift[None], residual, out_weight)


def experts_kernel(
    n_sp,
    n_tp,
    slots,
    extra,
    x_ref,
    routes_ref,
    prob_ref,
    logit_ref,
    gain_ref,
    shift_ref,
    gate_hbm,
    up_hbm,
    down_hbm,
    out_ref,
    w_in,
    w_out,
    place,
    outbox,
    inbox,
    partial,
    near_in,
    far_out,
    far_in,
    done,
    returned,
    rows_ref,
    load_sem,
    zs,
    zr,
    fs,
    fr,
    ns,
    nr,
    ps,
    pr,
    qs,
    qr,
    bs,
    br,
):
    me = lax.axis_index("sp")
    t = lax.axis_index("tp")
    near = t + 1 - 2 * lax.rem(t, 2)
    far = lax.rem(t + 2, 4)
    across = lax.rem(near + 2, 4)
    local, width = x_ref.shape
    hidden_width = w_out.shape[0]
    count = n_sp * n_tp
    f32, bf16 = jnp.float32, jnp.bfloat16
    step_cols = 1024 if width % 1024 == 0 else width

    loads = [
        pltpu.make_async_copy(gate_hbm.at[0], w_in.at[:, :hidden_width], load_sem.at[0]),
        pltpu.make_async_copy(up_hbm.at[0], w_in.at[:, hidden_width:], load_sem.at[1]),
        pltpu.make_async_copy(down_hbm.at[0], w_out, load_sem.at[2]),
    ]
    for load in loads:
        load.start()

    barrier = pltpu.get_barrier_semaphore()
    for step in range(1, n_sp):
        pl.semaphore_signal(
            barrier, inc=1, device_id={"sp": lax.rem(me + step, n_sp)}, device_id_type=MESH
        )
    for partner in (near, far):
        pl.semaphore_signal(barrier, inc=1, device_id={"tp": partner}, device_id_type=MESH)

    same = lax.broadcasted_iota(jnp.int32, (local, local), 0) == lax.broadcasted_iota(
        jnp.int32, (local, local), 1
    )

    def column(line_of):
        return jnp.sum(jnp.where(same, line_of, jnp.zeros_like(line_of)), axis=1, keepdims=True)

    first, second = column(routes_ref[0:1, :]), column(routes_ref[1:2, :])
    prob = column(prob_ref[...])
    line = lax.broadcasted_iota(jnp.int32, (local, n_sp), 1)
    member = jnp.where(
        (line == first // n_tp) | (line == second // n_tp), 1.0, 0.0
    ).astype(bf16)
    before = jnp.where(
        lax.broadcasted_iota(jnp.int32, (local, local), 1)
        < lax.broadcasted_iota(jnp.int32, (local, local), 0),
        1.0,
        0.0,
    ).astype(bf16)
    rank = jnp.dot(before, member, preferred_element_type=f32).astype(bf16)
    total = n_sp * slots
    spread = jnp.where(
        lax.broadcasted_iota(jnp.int32, (n_sp, total), 1) // slots
        == lax.broadcasted_iota(jnp.int32, (n_sp, total), 0),
        1.0,
        0.0,
    ).astype(bf16)
    member_wide = jnp.dot(member, spread, preferred_element_type=f32)
    rank_wide = jnp.dot(rank, spread, preferred_element_type=f32)
    slot_id = lax.rem(lax.broadcasted_iota(jnp.int32, (local, total), 1), slots).astype(f32)
    place[...] = jnp.where((member_wide > 0.5) & (rank_wide == slot_id), 1.0, 0.0).astype(bf16)

    difference = column(logit_ref[0:1, :] - logit_ref[1:2, :])
    weight_one = prob / (1.0 + jnp.exp(-difference))
    weight_two = prob / (1.0 + jnp.exp(difference))
    lane = lax.broadcasted_iota(jnp.int32, (local, extra), 1)
    name = lax.rem(lane, count)
    value = jnp.where(name == first, weight_one, 0.0) + jnp.where(name == second, weight_two, 0.0)
    value = jnp.where(lane < 2 * count, value, 0.0)
    high = value.astype(bf16)
    low = (value - high.astype(f32)).astype(bf16)
    tags = jnp.where(lane < count, high.astype(f32), low.astype(f32)).astype(bf16)

    def placed(rows):
        return lax.dot_general(
            place[...], rows, (((0,), (0,)), ((), ())), preferred_element_type=f32
        ).astype(bf16)

    for c in range(0, width, step_cols):
        outbox[:, :, c : c + step_cols] = placed(x_ref[:, c : c + step_cols]).reshape(
            n_sp, slots, step_cols
        )
    outbox[:, :, width:] = placed(tags).reshape(n_sp, slots, extra)

    pl.semaphore_wait(barrier, n_sp + 1)

    def go(z):
        return remote(outbox.at[z], inbox.at[me, t], zs.at[z], zr.at[me], {"sp": z})

    def come(z):
        return remote(outbox.at[z], inbox.at[z, t], zs.at[z], zr.at[z], {"sp": z})

    def to_far(z):
        return remote(inbox.at[z, t], inbox.at[z, t], fs.at[z], fr.at[z], {"tp": far})

    def to_near(z, i):
        block = inbox.at[z, (t, far)[i]]
        return remote(block, block, ns.at[z, i], nr.at[z, i], {"tp": near})

    def part_near(z, i):
        return remote(
            partial.at[z, (near, across)[i]],
            near_in.at[z, i],
            ps.at[z, i],
            pr.at[z, i],
            {"tp": near},
        )

    def part_far(z):
        return remote(far_out.at[z], far_in.at[z], qs.at[z], qr.at[z], {"tp": far})

    def back(z):
        return remote(done.at[z], returned.at[me], bs.at[z], br.at[me], {"sp": z})

    def back_in(z):
        return remote(done.at[z], returned.at[z], bs.at[z], br.at[z], {"sp": z})

    def pair(step):
        other, scale = 0, 1
        while scale < n_sp:
            bit = lax.rem(me // scale + step // scale, 2)
            other = other + bit * scale
            scale = 2 * scale
        return other

    def send_out(step, _):
        go(pair(step)).start()
        return 0

    lax.fori_loop(1, min(3, n_sp), send_out, 0)
    inbox[me, t] = outbox[me]

    def run_experts(z):
        rows = inbox[z].reshape(n_tp * slots, width + extra)
        own = me * n_tp + t
        tag = rows[:, width:].astype(f32)
        tag_lane = lax.broadcasted_iota(jnp.int32, tag.shape, 1)
        weight = jnp.sum(
            jnp.where((tag_lane == own) | (tag_lane == own + count), tag, 0.0),
            axis=1,
            keepdims=True,
        )
        both = jnp.dot(rows[:, :width], w_in[...], preferred_element_type=f32)
        gate, upper = both[:, :hidden_width], both[:, hidden_width:]
        hidden = (gate / (1.0 + jnp.exp(-gate)) * upper).astype(bf16)
        for c in range(0, width, step_cols):
            part = jnp.dot(
                hidden, w_out[:, c : c + step_cols], preferred_element_type=f32
            ).astype(bf16)
            partial[z, :, :, c : c + step_cols] = (
                (part.astype(f32) * weight).astype(bf16).reshape(n_tp, slots, step_cols)
            )

    def turn(step, _):
        @pl.when(step < n_sp)
        def _():
            z = pair(step)

            @pl.when(step > 0)
            def _():
                come(z).wait_recv()

            @pl.when((step > 1) & (step < n_sp - 1))
            def _():
                go(pair(step + 1)).start()

            to_far(z).start()
            to_near(z, 0).start()

        @pl.when(step == 1)
        def _():
            for load in loads:
                load.wait()

        @pl.when((step >= 1) & (step <= n_sp))
        def _():
            z = pair(step - 1)
            to_far(z).wait_recv()
            to_near(z, 1).start()
            to_near(z, 0).wait_recv()
            to_near(z, 1).wait_recv()
            run_experts(z)
            part_near(z, 1).start()
            part_near(z, 0).start()
            part_near(z, 1).wait_recv()
            far_out[z] = (partial[z, far].astype(f32) + near_in[z, 1].astype(f32)).astype(bf16)
            part_far(z).start()
            part_near(z, 0).wait_recv()

        @pl.when(step >= 2)
        def _():
            z = pair(step - 2)
            part_far(z).wait_recv()
            whole = (
                partial[z, t].astype(f32) + near_in[z, 0].astype(f32) + far_in[z].astype(f32)
            ).astype(bf16)

            @pl.when(z == me)
            def _():
                returned[me] = whole

            @pl.when(z != me)
            def _():
                done[z] = whole
                back(z).start()

        return 0

    lax.fori_loop(0, n_sp + 2, turn, 0)

    def collect(step, _):
        back_in(pair(step)).wait_recv()
        return 0

    lax.fori_loop(1, n_sp, collect, 0)
    for c in range(0, width, step_cols):
        span = slice(c, c + step_cols)
        moe = jnp.dot(
            place[...], returned[:, :, span].reshape(total, step_cols), preferred_element_type=f32
        )
        rows_ref[:, span] = residual_scale * x_ref[:, span].astype(f32) + moe
    out_ref[...] = norm_rows(rows_ref[...], gain_ref[...], shift_ref[...]).astype(bf16)

    def drain(step, _):
        z = pair(step)

        @pl.when(step > 0)
        def _():
            go(z).wait_send()
            back(z).wait_send()

        to_far(z).wait_send()
        part_far(z).wait_send()
        for i in range(2):
            to_near(z, i).wait_send()
            part_near(z, i).wait_send()
        return 0

    lax.fori_loop(0, n_sp, drain, 0)


def experts(normed, routes, group_prob, pair_logits, gain, shift, w_gate, w_up, w_down):
    n_sp, n_tp = lax.axis_size("sp"), lax.axis_size("tp")
    assert n_tp == 4 and n_sp & (n_sp - 1) == 0
    local, width = normed.shape
    hidden = w_down.shape[1]
    count = n_sp * n_tp
    group = count // GROUPS
    capacity = local // group
    slots = n_tp * capacity
    if n_tp % group == 0:
        slots = slots // TOPK
    extra = -(-2 * count // 128) * 128
    vmem = pl.BlockSpec(memory_space=pltpu.VMEM)
    hbm = pl.BlockSpec(memory_space=pl.ANY)
    dma = pltpu.SemaphoreType.DMA
    bf16, f32 = jnp.bfloat16, jnp.float32
    return pl.pallas_call(
        functools.partial(experts_kernel, n_sp, n_tp, slots, extra),
        out_shape=jax.ShapeDtypeStruct((local, width), bf16),
        in_specs=[vmem] * 6 + [hbm] * 3,
        out_specs=vmem,
        scratch_shapes=[
            pltpu.VMEM((width, 2 * hidden), bf16),
            pltpu.VMEM((hidden, width), bf16),
            pltpu.VMEM((local, n_sp * slots), bf16),
            pltpu.VMEM((n_sp, slots, width + extra), bf16),
            pltpu.VMEM((n_sp, n_tp, slots, width + extra), bf16),
            pltpu.VMEM((n_sp, n_tp, slots, width), bf16),
            pltpu.VMEM((n_sp, 2, slots, width), bf16),
            pltpu.VMEM((n_sp, slots, width), bf16),
            pltpu.VMEM((n_sp, slots, width), bf16),
            pltpu.VMEM((n_sp, slots, width), bf16),
            pltpu.VMEM((n_sp, slots, width), bf16),
            pltpu.VMEM((local, width), f32),
            dma((3,)),
            dma((n_sp,)),
            dma((n_sp,)),
            dma((n_sp,)),
            dma((n_sp,)),
            dma((n_sp, 2)),
            dma((n_sp, 2)),
            dma((n_sp, 2)),
            dma((n_sp, 2)),
            dma((n_sp,)),
            dma((n_sp,)),
            dma((n_sp,)),
            dma((n_sp,)),
        ],
        compiler_params=pltpu.CompilerParams(collective_id=1, has_side_effects=True),
        name="experts",
    )(
        normed,
        routes.T,
        group_prob[None],
        pair_logits.T,
        gain[None],
        shift[None],
        w_gate,
        w_up,
        w_down,
    )


def per_device(
    queries,
    keys,
    values,
    offsets,
    residual,
    out_weight,
    gain_one,
    shift_one,
    gain_two,
    shift_two,
    group_prob,
    pair_logits,
    routes,
    w_gate,
    w_up,
    w_down,
):
    normed = attend(
        queries, keys, values, offsets, residual, out_weight, gain_one, shift_one
    )
    return experts(
        normed, routes, group_prob, pair_logits, gain_two, shift_two, w_gate, w_up, w_down
    )


def solution(mesh):
    return jax.shard_map(
        per_device,
        mesh=mesh,
        in_specs=(
            P(("grp", "sp"), "tp"),
            P(("grp", "sp"), "tp"),
            P(("grp", "sp"), "tp"),
            P("tp"),
            P(("grp", "sp", "tp"), None),
            P("tp", None),
            P(),
            P(),
            P(),
            P(),
            P(("grp", "sp", "tp")),
            P(("grp", "sp", "tp"), None),
            P(("grp", "sp", "tp"), None),
            P(("sp", "tp"), None, None),
            P(("sp", "tp"), None, None),
            P(("sp", "tp"), None, None),
        ),
        out_specs=P(("grp", "sp", "tp"), None),
        check_vma=False,
    )
```

```python
import functools

import jax
import jax.numpy as jnp
from jax import lax
from jax.experimental import pallas as pl
from jax.experimental.pallas import tpu as pltpu
from jax.sharding import PartitionSpec as P

HEAD_DIM = 128
GROUPS = 4
TOPK = 2
MESH = pl.DeviceIdType.MESH

residual_scale = 8.0**0.25
norm_eps = 1e-05


def remote(src, dst, send_sem, recv_sem, target):
    return pltpu.make_async_remote_copy(
        src_ref=src,
        dst_ref=dst,
        send_sem=send_sem,
        recv_sem=recv_sem,
        device_id=target,
        device_id_type=MESH,
    )


def norm_rows(rows, gain, shift):
    mean = jnp.mean(rows, axis=-1, keepdims=True)
    centred = rows - mean
    variance = jnp.mean(centred * centred, axis=-1, keepdims=True)
    return centred * lax.rsqrt(variance + norm_eps) * gain + shift


def attend_kernel(
    n_sp,
    n_tp,
    chunks,
    off_ref,
    q_ref,
    k_ref,
    v_ref,
    gain_ref,
    shift_ref,
    res_hbm,
    w_hbm,
    out_ref,
    kv,
    w_ref,
    res_ref,
    later_ref,
    carry,
    acc,
    att,
    send1,
    keep1,
    recv1,
    send2,
    recv2,
    rows_ref,
    load_sem,
    kv_send,
    kv_recv,
    s1,
    r1,
    s2,
    r2,
):
    me = lax.axis_index("sp")
    t = lax.axis_index("tp")
    rows = q_ref.shape[0]
    heads = q_ref.shape[1] // HEAD_DIM
    local = res_ref.shape[0]
    cols = w_ref.shape[1] // chunks
    near = t + 1 - 2 * lax.rem(t, 2)
    far = lax.rem(t + 2, 4)

    load_w = pltpu.make_async_copy(w_hbm, w_ref, load_sem.at[0])
    load_res = pltpu.make_async_copy(res_hbm, res_ref, load_sem.at[1])
    load_w.start()
    load_res.start()

    barrier = pltpu.get_barrier_semaphore()
    for step in (1, n_sp - 1):
        pl.semaphore_signal(
            barrier, inc=1, device_id={"sp": lax.rem(me + step, n_sp)}, device_id_type=MESH
        )
    for partner in (near, far):
        pl.semaphore_signal(barrier, inc=1, device_id={"tp": partner}, device_id_type=MESH)
    pl.semaphore_wait(barrier, 4)

    up = {"sp": lax.rem(me + 1, n_sp)}
    own = [
        remote(ref, kv.at[me, i], kv_send.at[me, i], kv_recv.at[me, i], up)
        for i, ref in enumerate((k_ref, v_ref))
    ]

    def passed(j, i):
        return remote(kv.at[j, i], kv.at[j, i], kv_send.at[j, i], kv_recv.at[j, i], up)

    @pl.when(me < n_sp - 1)
    def _():
        own[0].start()
        own[1].start()

    row_id = lax.broadcasted_iota(jnp.int32, (rows, rows), 0)
    col_id = lax.broadcasted_iota(jnp.int32, (rows, rows), 1)
    later_ref[...] = jnp.where(row_id > col_id, 1.0, 0.0).astype(jnp.bfloat16)
    scale = HEAD_DIM ** (-0.5)

    def block(key_of, value_of, first):
        for h in range(heads):
            span = slice(h * HEAD_DIM, (h + 1) * HEAD_DIM)
            score = (
                lax.dot_general(
                    q_ref[:, span],
                    key_of(span),
                    (((1,), (1,)), ((), ())),
                    preferred_element_type=jnp.float32,
                )
                * scale
                - off_ref[h]
            )
            soft = jnp.maximum(score, 0.0) + jnp.log(1.0 + jnp.exp(-jnp.abs(score)))
            gain = score - soft
            if first:
                soft = jnp.where(col_id < row_id, soft, 0.0)
            high = soft.astype(jnp.bfloat16)
            low = (soft - high.astype(jnp.float32)).astype(jnp.bfloat16)
            tail = jnp.dot(high, later_ref[...], preferred_element_type=jnp.float32)
            tail = tail + jnp.dot(low, later_ref[...], preferred_element_type=jnp.float32)
            total = jnp.sum(soft, axis=1, keepdims=True)
            if first:
                weight = jnp.where(col_id < row_id, jnp.exp(gain - tail), 0.0)
                carry[h] = total
            else:
                weight = jnp.exp(gain - tail - carry[h])
                carry[h] = carry[h] + total
            part = jnp.dot(
                weight.astype(jnp.bfloat16), value_of(span), preferred_element_type=jnp.float32
            )
            if first:
                acc[:, span] = part
            else:
                acc[:, span] = acc[:, span] + part

    block(lambda span: k_ref[:, span], lambda span: v_ref[:, span], True)

    def turn(step, _):
        j = me - step
        for i in range(2):
            passed(j, i).wait_recv()

            @pl.when(me < n_sp - 1)
            def _():
                passed(j, i).start()

        block(lambda span: kv[j, 0, :, span], lambda span: kv[j, 1, :, span], False)
        return 0

    lax.fori_loop(1, me + 1, turn, 0)

    att[...] = acc[...].astype(jnp.bfloat16)
    order = (
        near + 2 - 4 * (near // 2),
        near,
        far,
        t,
    )
    picked = jnp.concatenate(
        [att[pl.ds(pl.multiple_of(b * local, local), local), :] for b in order], axis=0
    )
    half = rows // 2
    load_w.wait()
    load_res.wait()

    def hop1(c):
        return remote(send1.at[c], recv1.at[c], s1.at[c], r1.at[c], {"tp": near})

    def hop2(c):
        return remote(send2.at[c], recv2.at[c], s2.at[c], r2.at[c], {"tp": far})

    for c in range(chunks):
        part = jnp.dot(
            picked, w_ref[:, c * cols : (c + 1) * cols], preferred_element_type=jnp.float32
        ).astype(jnp.bfloat16)
        send1[c] = part[:half]
        keep1[c] = part[half:]
        hop1(c).start()
    for c in range(chunks):
        hop1(c).wait_recv()
        both = keep1[c].astype(jnp.float32) + recv1[c].astype(jnp.float32)
        send2[c] = both[:local].astype(jnp.bfloat16)
        hop2(c).start()
        span = slice(c * cols, (c + 1) * cols)
        rows_ref[:, span] = (
            residual_scale * res_ref[:, span].astype(jnp.float32) + both[local:]
        )
    for c in range(chunks):
        hop2(c).wait_recv()
        span = slice(c * cols, (c + 1) * cols)
        rows_ref[:, span] = rows_ref[:, span] + recv2[c].astype(jnp.float32)
    out_ref[...] = norm_rows(rows_ref[...], gain_ref[...], shift_ref[...]).astype(jnp.bfloat16)

    for c in range(chunks):
        hop1(c).wait_send()
        hop2(c).wait_send()

    @pl.when(me < n_sp - 1)
    def _():
        own[0].wait_send()
        own[1].wait_send()

        def drain(step, _):
            for i in range(2):
                passed(me - step, i).wait_send()
            return 0

        lax.fori_loop(1, me + 1, drain, 0)


def attend(queries, keys, values, offsets, residual, out_weight, gain, shift):
    n_sp, n_tp = lax.axis_size("sp"), lax.axis_size("tp")
    assert n_tp == 4
    rows, inner = queries.shape
    local, width = residual.shape
    heads = offsets.shape[0]
    chunks = 8
    cols = width // chunks
    half = rows // 2
    vmem = pl.BlockSpec(memory_space=pltpu.VMEM)
    hbm = pl.BlockSpec(memory_space=pl.ANY)
    dma = pltpu.SemaphoreType.DMA
    bf16, f32 = jnp.bfloat16, jnp.float32
    return pl.pallas_call(
        functools.partial(attend_kernel, n_sp, n_tp, chunks),
        out_shape=jax.ShapeDtypeStruct((local, width), bf16),
        in_specs=[pl.BlockSpec(memory_space=pltpu.SMEM), vmem, vmem, vmem, vmem, vmem, hbm, hbm],
        out_specs=vmem,
        scratch_shapes=[
            pltpu.VMEM((n_sp, 2, rows, inner), bf16),
            pltpu.VMEM(out_weight.shape, bf16),
            pltpu.VMEM(residual.shape, bf16),
            pltpu.VMEM((rows, rows), bf16),
            pltpu.VMEM((heads, rows, 1), f32),
            pltpu.VMEM((rows, inner), f32),
            pltpu.VMEM((rows, inner), bf16),
            pltpu.VMEM((chunks, half, cols), bf16),
            pltpu.VMEM((chunks, half, cols), bf16),
            pltpu.VMEM((chunks, half, cols), bf16),
            pltpu.VMEM((chunks, local, cols), bf16),
            pltpu.VMEM((chunks, local, cols), bf16),
            pltpu.VMEM((local, width), f32),
            dma((2,)),
            dma((n_sp, 2)),
            dma((n_sp, 2)),
            dma((chunks,)),
            dma((chunks,)),
            dma((chunks,)),
            dma((chunks,)),
        ],
        compiler_params=pltpu.CompilerParams(collective_id=0, has_side_effects=True),
        name="attend",
    )(offsets, queries, keys, values, gain[None], shift[None], residual, out_weight)


def experts_kernel(
    n_sp,
    n_tp,
    slots,
    extra,
    x_ref,
    routes_ref,
    prob_ref,
    logit_ref,
    gain_ref,
    shift_ref,
    gate_hbm,
    up_hbm,
    down_hbm,
    out_ref,
    w_in,
    w_out,
    place,
    outbox,
    inbox,
    partial,
    near_in,
    far_out,
    far_in,
    done,
    returned,
    rows_ref,
    load_sem,
    zs,
    zr,
    fs,
    fr,
    ns,
    nr,
    ps,
    pr,
    qs,
    qr,
    bs,
    br,
):
    me = lax.axis_index("sp")
    t = lax.axis_index("tp")
    near = t + 1 - 2 * lax.rem(t, 2)
    far = lax.rem(t + 2, 4)
    across = lax.rem(near + 2, 4)
    local, width = x_ref.shape
    hidden_width = w_out.shape[0]
    count = n_sp * n_tp
    f32, bf16 = jnp.float32, jnp.bfloat16
    step_cols = 1024 if width % 1024 == 0 else width

    loads = [
        pltpu.make_async_copy(gate_hbm.at[0], w_in.at[:, :hidden_width], load_sem.at[0]),
        pltpu.make_async_copy(up_hbm.at[0], w_in.at[:, hidden_width:], load_sem.at[1]),
        pltpu.make_async_copy(down_hbm.at[0], w_out, load_sem.at[2]),
    ]
    for load in loads:
        load.start()

    barrier = pltpu.get_barrier_semaphore()
    for step in range(1, n_sp):
        pl.semaphore_signal(
            barrier, inc=1, device_id={"sp": lax.rem(me + step, n_sp)}, device_id_type=MESH
        )
    for partner in (near, far):
        pl.semaphore_signal(barrier, inc=1, device_id={"tp": partner}, device_id_type=MESH)

    same = lax.broadcasted_iota(jnp.int32, (local, local), 0) == lax.broadcasted_iota(
        jnp.int32, (local, local), 1
    )

    def column(line_of):
        return jnp.sum(jnp.where(same, line_of, jnp.zeros_like(line_of)), axis=1, keepdims=True)

    first, second = column(routes_ref[0:1, :]), column(routes_ref[1:2, :])
    prob = column(prob_ref[...])
    line = lax.broadcasted_iota(jnp.int32, (local, n_sp), 1)
    member = jnp.where(
        (line == first // n_tp) | (line == second // n_tp), 1.0, 0.0
    ).astype(bf16)
    before = jnp.where(
        lax.broadcasted_iota(jnp.int32, (local, local), 1)
        < lax.broadcasted_iota(jnp.int32, (local, local), 0),
        1.0,
        0.0,
    ).astype(bf16)
    rank = jnp.dot(before, member, preferred_element_type=f32).astype(bf16)
    total = n_sp * slots
    spread = jnp.where(
        lax.broadcasted_iota(jnp.int32, (n_sp, total), 1) // slots
        == lax.broadcasted_iota(jnp.int32, (n_sp, total), 0),
        1.0,
        0.0,
    ).astype(bf16)
    member_wide = jnp.dot(member, spread, preferred_element_type=f32)
    rank_wide = jnp.dot(rank, spread, preferred_element_type=f32)
    slot_id = lax.rem(lax.broadcasted_iota(jnp.int32, (local, total), 1), slots).astype(f32)
    place[...] = jnp.where((member_wide > 0.5) & (rank_wide == slot_id), 1.0, 0.0).astype(bf16)

    difference = column(logit_ref[0:1, :] - logit_ref[1:2, :])
    weight_one = prob / (1.0 + jnp.exp(-difference))
    weight_two = prob / (1.0 + jnp.exp(difference))
    lane = lax.broadcasted_iota(jnp.int32, (local, extra), 1)
    name = lax.rem(lane, count)
    value = jnp.where(name == first, weight_one, 0.0) + jnp.where(name == second, weight_two, 0.0)
    value = jnp.where(lane < 2 * count, value, 0.0)
    high = value.astype(bf16)
    low = (value - high.astype(f32)).astype(bf16)
    tags = jnp.where(lane < count, high.astype(f32), low.astype(f32)).astype(bf16)

    def placed(rows):
        return lax.dot_general(
            place[...], rows, (((0,), (0,)), ((), ())), preferred_element_type=f32
        ).astype(bf16)

    for c in range(0, width, step_cols):
        outbox[:, :, c : c + step_cols] = placed(x_ref[:, c : c + step_cols]).reshape(
            n_sp, slots, step_cols
        )
    outbox[:, :, width:] = placed(tags).reshape(n_sp, slots, extra)

    pl.semaphore_wait(barrier, n_sp + 1)

    def go(z):
        return remote(outbox.at[z], inbox.at[me, t], zs.at[z], zr.at[me], {"sp": z})

    def come(z):
        return remote(outbox.at[z], inbox.at[z, t], zs.at[z], zr.at[z], {"sp": z})

    def to_far(z):
        return remote(inbox.at[z, t], inbox.at[z, t], fs.at[z], fr.at[z], {"tp": far})

    def to_near(z, i):
        block = inbox.at[z, (t, far)[i]]
        return remote(block, block, ns.at[z, i], nr.at[z, i], {"tp": near})

    def part_near(z, i):
        return remote(
            partial.at[z, (near, across)[i]],
            near_in.at[z, i],
            ps.at[z, i],
            pr.at[z, i],
            {"tp": near},
        )

    def part_far(z):
        return remote(far_out.at[z], far_in.at[z], qs.at[z], qr.at[z], {"tp": far})

    def back(z):
        return remote(done.at[z], returned.at[me], bs.at[z], br.at[me], {"sp": z})

    def back_in(z):
        return remote(done.at[z], returned.at[z], bs.at[z], br.at[z], {"sp": z})

    def pair(step):
        other, scale = 0, 1
        while scale < n_sp:
            bit = lax.rem(me // scale + step // scale, 2)
            other = other + bit * scale
            scale = 2 * scale
        return other

    def send_out(step, _):
        go(pair(step)).start()
        return 0

    lax.fori_loop(1, min(3, n_sp), send_out, 0)
    inbox[me, t] = outbox[me]

    def run_experts(z):
        rows = inbox[z].reshape(n_tp * slots, width + extra)
        own = me * n_tp + t
        tag = rows[:, width:].astype(f32)
        tag_lane = lax.broadcasted_iota(jnp.int32, tag.shape, 1)
        weight = jnp.sum(
            jnp.where((tag_lane == own) | (tag_lane == own + count), tag, 0.0),
            axis=1,
            keepdims=True,
        )
        both = jnp.dot(rows[:, :width], w_in[...], preferred_element_type=f32)
        gate, upper = both[:, :hidden_width], both[:, hidden_width:]
        hidden = (gate / (1.0 + jnp.exp(-gate)) * upper).astype(bf16)
        for c in range(0, width, step_cols):
            part = jnp.dot(
                hidden, w_out[:, c : c + step_cols], preferred_element_type=f32
            ).astype(bf16)
            partial[z, :, :, c : c + step_cols] = (
                (part.astype(f32) * weight).astype(bf16).reshape(n_tp, slots, step_cols)
            )

    def turn(step, _):
        @pl.when(step < n_sp)
        def _():
            z = pair(step)

            @pl.when(step > 0)
            def _():
                come(z).wait_recv()

            @pl.when((step > 0) & (step < n_sp - 2))
            def _():
                go(pair(step + 2)).start()

            to_far(z).start()
            to_near(z, 0).start()

        @pl.when(step == 1)
        def _():
            for load in loads:
                load.wait()

        @pl.when((step >= 1) & (step <= n_sp))
        def _():
            z = pair(step - 1)
            to_far(z).wait_recv()
            to_near(z, 1).start()
            to_near(z, 0).wait_recv()
            to_near(z, 1).wait_recv()
            run_experts(z)
            part_near(z, 1).start()
            part_near(z, 0).start()
            part_near(z, 1).wait_recv()
            far_out[z] = (partial[z, far].astype(f32) + near_in[z, 1].astype(f32)).astype(bf16)
            part_far(z).start()
            part_near(z, 0).wait_recv()

        @pl.when(step >= 2)
        def _():
            z = pair(step - 2)
            part_far(z).wait_recv()
            whole = (
                partial[z, t].astype(f32) + near_in[z, 0].astype(f32) + far_in[z].astype(f32)
            ).astype(bf16)

            @pl.when(z == me)
            def _():
                returned[me] = whole

            @pl.when(z != me)
            def _():
                done[z] = whole
                back(z).start()

        return 0

    lax.fori_loop(0, n_sp + 2, turn, 0)

    def collect(step, _):
        back_in(pair(step)).wait_recv()
        return 0

    lax.fori_loop(1, n_sp, collect, 0)
    for c in range(0, width, step_cols):
        span = slice(c, c + step_cols)
        moe = jnp.dot(
            place[...], returned[:, :, span].reshape(total, step_cols), preferred_element_type=f32
        )
        rows_ref[:, span] = residual_scale * x_ref[:, span].astype(f32) + moe
    out_ref[...] = norm_rows(rows_ref[...], gain_ref[...], shift_ref[...]).astype(bf16)

    def drain(step, _):
        z = pair(step)

        @pl.when(step > 0)
        def _():
            go(z).wait_send()
            back(z).wait_send()

        to_far(z).wait_send()
        part_far(z).wait_send()
        for i in range(2):
            to_near(z, i).wait_send()
            part_near(z, i).wait_send()
        return 0

    lax.fori_loop(0, n_sp, drain, 0)


def experts(normed, routes, group_prob, pair_logits, gain, shift, w_gate, w_up, w_down):
    n_sp, n_tp = lax.axis_size("sp"), lax.axis_size("tp")
    assert n_tp == 4 and n_sp & (n_sp - 1) == 0
    local, width = normed.shape
    hidden = w_down.shape[1]
    count = n_sp * n_tp
    group = count // GROUPS
    capacity = local // group
    slots = n_tp * capacity
    if n_tp % group == 0:
        slots = slots // TOPK
    extra = -(-2 * count // 128) * 128
    vmem = pl.BlockSpec(memory_space=pltpu.VMEM)
    hbm = pl.BlockSpec(memory_space=pl.ANY)
    dma = pltpu.SemaphoreType.DMA
    bf16, f32 = jnp.bfloat16, jnp.float32
    return pl.pallas_call(
        functools.partial(experts_kernel, n_sp, n_tp, slots, extra),
        out_shape=jax.ShapeDtypeStruct((local, width), bf16),
        in_specs=[vmem] * 6 + [hbm] * 3,
        out_specs=vmem,
        scratch_shapes=[
            pltpu.VMEM((width, 2 * hidden), bf16),
            pltpu.VMEM((hidden, width), bf16),
            pltpu.VMEM((local, n_sp * slots), bf16),
            pltpu.VMEM((n_sp, slots, width + extra), bf16),
            pltpu.VMEM((n_sp, n_tp, slots, width + extra), bf16),
            pltpu.VMEM((n_sp, n_tp, slots, width), bf16),
            pltpu.VMEM((n_sp, 2, slots, width), bf16),
            pltpu.VMEM((n_sp, slots, width), bf16),
            pltpu.VMEM((n_sp, slots, width), bf16),
            pltpu.VMEM((n_sp, slots, width), bf16),
            pltpu.VMEM((n_sp, slots, width), bf16),
            pltpu.VMEM((local, width), f32),
            dma((3,)),
            dma((n_sp,)),
            dma((n_sp,)),
            dma((n_sp,)),
            dma((n_sp,)),
            dma((n_sp, 2)),
            dma((n_sp, 2)),
            dma((n_sp, 2)),
            dma((n_sp, 2)),
            dma((n_sp,)),
            dma((n_sp,)),
            dma((n_sp,)),
            dma((n_sp,)),
        ],
        compiler_params=pltpu.CompilerParams(collective_id=1, has_side_effects=True),
        name="experts",
    )(
        normed,
        routes.T,
        group_prob[None],
        pair_logits.T,
        gain[None],
        shift[None],
        w_gate,
        w_up,
        w_down,
    )


def per_device(
    queries,
    keys,
    values,
    offsets,
    residual,
    out_weight,
    gain_one,
    shift_one,
    gain_two,
    shift_two,
    group_prob,
    pair_logits,
    routes,
    w_gate,
    w_up,
    w_down,
):
    normed = attend(
        queries, keys, values, offsets, residual, out_weight, gain_one, shift_one
    )
    return experts(
        normed, routes, group_prob, pair_logits, gain_two, shift_two, w_gate, w_up, w_down
    )


def solution(mesh):
    return jax.shard_map(
        per_device,
        mesh=mesh,
        in_specs=(
            P(("grp", "sp"), "tp"),
            P(("grp", "sp"), "tp"),
            P(("grp", "sp"), "tp"),
            P("tp"),
            P(("grp", "sp", "tp"), None),
            P("tp", None),
            P(),
            P(),
            P(),
            P(),
            P(("grp", "sp", "tp")),
            P(("grp", "sp", "tp"), None),
            P(("grp", "sp", "tp"), None),
            P(("sp", "tp"), None, None),
            P(("sp", "tp"), None, None),
            P(("sp", "tp"), None, None),
        ),
        out_specs=P(("grp", "sp", "tp"), None),
        check_vma=False,
    )
```
